32 devices in a mesh: fs: 8 (over z, core), tp: 4 (over y, x).
Axes of the slice: x: 2, y: 2, z: 4, core: 2. Of those that a mesh axis runs over, the one named last changes fastest.
Arguments:
- prompt: bfloat16 [1024, 2048], P('tp'), may hold values from -6 to 6
- norm_gain: float32 [2048], P('fs'), may hold values from 0.1 to 1.9
- gate_master: float32 [32, 2048, 512], P(None, 'fs', 'tp'), may hold values from -6 to 6
- up_master: float32 [32, 2048, 512], P(None, 'fs', 'tp'), may hold values from -6 to 6
- down_master: float32 [32, 2048, 512], P(None, 'fs', 'tp'), may hold values from -6 to 6
- group_choice: int32 [1024], P('tp'), may hold values from 0 to 3
- inner_choice: int32 [1024, 2], P('tp'), may hold values from 0 to 7, as said below
- route_weight: float32 [1024, 2], P('tp'), may hold values from 0.2 to 1
Outputs:
- gate_served: bfloat16 [2048, 16384], P(None, 'fs')
- up_served: bfloat16 [2048, 16384], P(None, 'fs')
- down_served: bfloat16 [2048, 16384], P(None, 'fs')
- mixed: bfloat16 [1024, 2048], P('tp', 'fs')
The draws below stay inside these ranges and needn't reach their ends.
Inputs may be any that keep to these rules, and one draw needn't show every extreme that they name: `inner_choice`: the two experts of a token differ.
All inputs are finite; a program needn't handle non-finite values.
Results may differ from the reference program's by a relative error of at most 0.0081.
Values may be sent and summed in bfloat16 or wider, within the bound.
No kernel may reach another device: no remote copies, remote signals or barrier semaphores. Data moves between devices by JAX's collectives and lax.ppermute only.
A program may use at most 128 MiB of HBM per device.

```python
import math
import jax
import jax.numpy as jnp
from jax import lax

D = 2048
FF = 512
GROUPS = 4
EPG = 8
TOK_DEV = 256
EXPERTS = 32
TOKENS = 1024


def routing_draw(key):
    base = jax.random.fold_in(key, 7411)
    keys = jax.random.split(base, 9)
    shards = TOKENS // TOK_DEV
    hot_group = jax.random.randint(keys[0], (shards,), 0, GROUPS)
    hot_inner = jax.random.randint(keys[1], (shards,), 0, EPG)
    hot_count = jax.random.randint(keys[2], (shards,), 0, TOK_DEV // 2 + 1)
    heavy = jax.random.randint(keys[3], (), 0, shards)
    hot_count = jnp.where(jnp.arange(shards) == heavy, 3 * TOK_DEV // 4, hot_count)
    ranks = jax.vmap(lambda sub: jax.random.permutation(sub, TOK_DEV))(jax.random.split(keys[4], shards))
    hot = (ranks < hot_count[:, None]).reshape(TOKENS)
    shard_of = jnp.arange(TOKENS) // TOK_DEV
    drawn_group = jax.random.randint(keys[5], (TOKENS,), 0, GROUPS)
    first_drawn = jax.random.randint(keys[6], (TOKENS,), 0, EPG)
    offsets = jax.random.randint(keys[7], (TOKENS,), 1, EPG)
    flip = jax.random.randint(keys[8], (TOKENS,), 0, 2)
    group = jnp.where(hot, hot_group[shard_of], drawn_group)
    first = jnp.where(hot, hot_inner[shard_of], first_drawn)
    second = (first + offsets) % EPG
    pair = jnp.where(flip[:, None] == 1, jnp.stack([second, first], axis=1), jnp.stack([first, second], axis=1))
    return (group.astype(jnp.int32), pair.astype(jnp.int32))


def draw_group_choice(key, part):
    group, pair = routing_draw(key)
    return group


def draw_inner_choice(key, part):
    group, pair = routing_draw(key)
    return pair


def levels(key, shape, cuts, smallest, high):
    def one(dim, blocks):
        steps = jax.random.uniform(jax.random.fold_in(jax.random.fold_in(key, 6), dim), (blocks,), jnp.float32, smallest / len(cuts), high / len(cuts))
        return jnp.repeat(jnp.exp(steps), shape[dim] // blocks).reshape((-1,) + (1,) * (len(shape) - dim - 1))

    loudness = one(*cuts[0])
    for cut in cuts[1:]:
        loudness = loudness * one(*cut)
    return loudness


def scatter_about(rng, extent, scale, reach, pieces=(), kind=jnp.bfloat16):
    drawn = jax.random.normal(rng, extent, jnp.float32) * scale
    if len(pieces) > 0:
        drawn = levels(rng, extent, pieces, -0.22, 0.18) * drawn
    return jnp.clip(drawn, min=-reach, max=reach).astype(kind)


def setup_inputs(seed: int = 0) -> dict:
    seeds = jax.random.split(jax.random.key(seed), 9)
    prompt = scatter_about(seeds[0], (TOKENS, D), 1.0, 6.0, ((0, 4),))
    norm_gain = jnp.clip(1.0 + 0.18 * jax.random.normal(seeds[1], (D,), jnp.float32), 0.1, 1.9)
    gate_master = scatter_about(seeds[2], (EXPERTS, D, FF), 1.0, 6.0, ((1, 8), (2, 4)), jnp.float32)
    up_master = scatter_about(seeds[3], (EXPERTS, D, FF), 1.0, 6.0, ((1, 8), (2, 4)), jnp.float32)
    down_master = scatter_about(seeds[4], (EXPERTS, D, FF), 1.0, 6.0, ((1, 8), (2, 4)), jnp.float32)
    group_choice = draw_group_choice(jax.random.fold_in(seeds[8], 71), 0)
    inner_choice = draw_inner_choice(jax.random.fold_in(seeds[8], 71), 0)
    route_weight = jnp.clip(jnp.exp(math.log(1.0) - 1.609438 * jax.random.uniform(seeds[7], (TOKENS, 2), jnp.float32) ** levels(seeds[7], (TOKENS, 2), ((0, 4),), -0.2, 0.2)), 0.2, 1.0)
    return dict(prompt=prompt, norm_gain=norm_gain, gate_master=gate_master, up_master=up_master, down_master=down_master, group_choice=group_choice, inner_choice=inner_choice, route_weight=route_weight)


def reference(prompt, norm_gain, gate_master, up_master, down_master, group_choice, inner_choice, route_weight):
    experts = GROUPS * EPG
    scale = norm_gain[None, :, None]
    gate_served = (gate_master * scale).astype(jnp.bfloat16).transpose(1, 0, 2).reshape(D, experts * FF)
    up_served = (up_master * scale).astype(jnp.bfloat16).transpose(1, 0, 2).reshape(D, experts * FF)
    down_served = down_master.astype(jnp.bfloat16).transpose(1, 0, 2).reshape(D, experts * FF)
    values = prompt.astype(jnp.float32)
    normed = (values * lax.rsqrt(lax.optimization_barrier(jnp.mean(values * values, axis=1, keepdims=True)) + 1e-06)).astype(jnp.bfloat16)
    chosen = group_choice[:, None] * EPG + inner_choice
    member = (chosen[:, :, None] == jnp.arange(experts, dtype=jnp.int32)[None, None, :]).astype(jnp.float32)
    weight = lax.optimization_barrier(jnp.sum(member * route_weight[:, :, None], axis=1))

    def one_expert(total, index):
        begin = (index * FF).astype(jnp.int32)
        gate_cols = lax.dynamic_slice_in_dim(gate_served, begin, FF, 1)
        up_cols = lax.dynamic_slice_in_dim(up_served, begin, FF, 1)
        down_cols = lax.dynamic_slice_in_dim(down_served, begin, FF, 1)
        gate_act = jnp.dot(normed, gate_cols, preferred_element_type=jnp.float32) * D ** (-0.5)
        up_act = jnp.dot(normed, up_cols, preferred_element_type=jnp.float32) * D ** (-0.5)
        column = lax.dynamic_slice_in_dim(weight, index.astype(jnp.int32), 1, 1)
        scaled = (column * jax.nn.silu(gate_act) * up_act).astype(jnp.bfloat16)
        part = lax.dot_general(scaled, down_cols, (((1,), (1,)), ((), ())), preferred_element_type=jnp.float32)
        return (total + part, None)
    total, _ = lax.scan(one_expert, jnp.zeros((prompt.shape[0], D), jnp.float32), jnp.arange(experts, dtype=jnp.int32))
    mixed = (total * FF ** (-0.5)).astype(jnp.bfloat16)
    return (gate_served, up_served, down_served, mixed)
```

```python
import functools

import jax
import jax.numpy as jnp
from jax import lax
from jax.experimental import pallas as pl
from jax.experimental.pallas import tpu as pltpu
from jax.sharding import PartitionSpec as P

FF = 512
GROUPS = 4
EPG = 8
LANES = 128


def flatten_rows(piece):
    count, experts, rows, hidden = piece.shape
    return piece.transpose(0, 2, 1, 3).reshape(count, rows, experts * hidden)


def restore_rows(gathered, rows):
    parts = lax.axis_size("tp")
    count, total, width = gathered.shape
    blocks = total // (parts * rows)
    ordered = gathered.reshape(count, parts, blocks, rows, width).transpose(0, 2, 1, 3, 4)
    return ordered.reshape(count, total, width)


def activations(normed, gate_local, up_local, column_weight):
    width = normed.shape[1]
    gate_act = jnp.dot(normed, gate_local, preferred_element_type=jnp.float32) * width ** (-0.5)
    up_act = jnp.dot(normed, up_local, preferred_element_type=jnp.float32) * width ** (-0.5)
    return (column_weight * jax.nn.silu(gate_act) * up_act).astype(jnp.bfloat16)


def route_columns(group_choice, inner_choice, route_weight, columns):
    first = lax.axis_index("fs") * columns
    owner = (first + jnp.arange(columns, dtype=jnp.int32)) // FF
    chosen = group_choice[:, None] * EPG + inner_choice
    picked = jnp.where(chosen[:, :, None] == owner[None, None, :], route_weight[:, :, None], 0.0)
    return jnp.sum(picked, axis=1)


def normalize(prompt):
    values = prompt.astype(jnp.float32)
    mean = jnp.mean(values * values, axis=1, keepdims=True)
    return (values * lax.rsqrt(mean + 1e-06)).astype(jnp.bfloat16)


def general_shards(
    prompt, norm_gain, gate_master, up_master, down_master, group_choice, inner_choice, route_weight
):
    scale = norm_gain[None, :, None]
    gate_cast = (gate_master * scale).astype(jnp.bfloat16)
    up_cast = (up_master * scale).astype(jnp.bfloat16)
    down_cast = down_master.astype(jnp.bfloat16)
    rows = gate_master.shape[1] // lax.axis_size("tp")
    normed = normalize(prompt)
    stacked = jnp.stack([gate_cast, up_cast, down_cast])
    widened = lax.all_to_all(stacked, "tp", split_axis=2, concat_axis=3, tiled=True)
    moved = lax.all_to_all(flatten_rows(widened), "fs", split_axis=2, concat_axis=1, tiled=True)
    served = restore_rows(lax.all_gather(moved, "tp", axis=1, tiled=True), rows)
    gate_local, up_local, down_local = (served[0], served[1], served[2])
    column_weight = route_columns(group_choice, inner_choice, route_weight, gate_local.shape[1])
    scaled = activations(normed, gate_local, up_local, column_weight)
    summed = lax.psum_scatter(
        lax.dot_general(
            down_local, scaled, (((1,), (1,)), ((), ())), preferred_element_type=jnp.float32
        ),
        "fs",
        scatter_dimension=0,
        tiled=True,
    )
    mixed = (summed * FF ** (-0.5)).T.astype(jnp.bfloat16)
    return (gate_local, up_local, down_local, mixed)


def cast_kernel(where_ref, gain_ref, gate_ref, up_ref, out_ref):
    gain = gain_ref[...]
    out_ref[0, 0] = (gate_ref[0] * gain).astype(jnp.bfloat16)
    out_ref[1, 0] = (up_ref[0] * gain).astype(jnp.bfloat16)


def cast_pair(block, gain, gate_master, up_master, held):
    _, rows, hidden = gate_master.shape
    source = pl.BlockSpec((1, rows, hidden), lambda e, where: (where[0] * held + e, 0, 0))
    return pl.pallas_call(
        cast_kernel,
        grid_spec=pltpu.PrefetchScalarGridSpec(
            num_scalar_prefetch=1,
            grid=(held,),
            in_specs=[pl.BlockSpec((rows, hidden), lambda e, where: (0, 0)), source, source],
            out_specs=pl.BlockSpec((2, 1, rows, hidden), lambda e, where: (0, e, 0, 0)),
        ),
        out_shape=jax.ShapeDtypeStruct((2, held, rows, hidden), jnp.bfloat16),
    )(block[None], gain, gate_master, up_master)


def lay_columns(parts, me, out_ref, pick, hidden):
    for step, part in enumerate(parts):
        column = pl.multiple_of((me ^ step) * hidden, LANES)
        out_ref[:, pl.ds(column, hidden)] = pick(part)


def lay_pair_kernel(where_ref, *refs, hidden, fresh):
    parts, outs = refs[:4], refs[4 if fresh else 6 :]
    for which, out_ref in enumerate(outs):
        lay_columns(parts, where_ref[1], out_ref, lambda part: part[which, 0], hidden)


def lay_pair(where, parts, outs, total):
    _, held, rows, hidden = parts[0].shape
    width = 4 * hidden
    fresh = outs is None
    part_spec = pl.BlockSpec((2, 1, rows, hidden), lambda e, where: (0, e, 0, 0))
    out_spec = pl.BlockSpec((rows, width), lambda e, where: (where[0], e))
    shape = jax.ShapeDtypeStruct((total, held * width), jnp.bfloat16)
    return pl.pallas_call(
        functools.partial(lay_pair_kernel, hidden=hidden, fresh=fresh),
        grid_spec=pltpu.PrefetchScalarGridSpec(
            num_scalar_prefetch=1,
            grid=(held,),
            in_specs=[part_spec] * 4 + [pl.BlockSpec(memory_space=pl.ANY)] * (0 if fresh else 2),
            out_specs=[out_spec, out_spec],
        ),
        out_shape=[shape, shape],
        input_output_aliases={} if fresh else {5: 0, 6: 1},
    )(where, *parts, *(() if fresh else outs))


def lay_down_kernel(where_ref, *refs, hidden, fresh):
    parts, scaled_ref = refs[:4], refs[4]
    out_ref, partial_ref = refs[5 if fresh else 6 :]
    lay_columns(parts, where_ref[1], out_ref, lambda part: part[0], hidden)
    product = lax.dot_general(
        scaled_ref[...], out_ref[...], (((1,), (1,)), ((), ())), preferred_element_type=jnp.float32
    )

    @pl.when(pl.program_id(0) == 0)
    def _():
        partial_ref[...] = product

    @pl.when(pl.program_id(0) > 0)
    def _():
        partial_ref[...] += product


def lay_down(where, parts, scaled, out, total):
    held, rows, hidden = parts[0].shape
    width = 4 * hidden
    tokens = scaled.shape[0]
    fresh = out is None
    part_spec = pl.BlockSpec((1, rows, hidden), lambda e, where: (e, 0, 0))
    return pl.pallas_call(
        functools.partial(lay_down_kernel, hidden=hidden, fresh=fresh),
        grid_spec=pltpu.PrefetchScalarGridSpec(
            num_scalar_prefetch=1,
            grid=(held,),
            in_specs=[part_spec] * 4
            + [pl.BlockSpec((tokens, width), lambda e, where: (0, e))]
            + [pl.BlockSpec(memory_space=pl.ANY)] * (0 if fresh else 1),
            out_specs=[
                pl.BlockSpec((rows, width), lambda e, where: (where[0], e)),
                pl.BlockSpec((tokens, rows), lambda e, where: (0, 0)),
            ],
        ),
        out_shape=[
            jax.ShapeDtypeStruct((total, held * width), jnp.bfloat16),
            jax.ShapeDtypeStruct((tokens, rows), jnp.float32),
        ],
        input_output_aliases={} if fresh else {6: 0},
    )(where, *parts, scaled, *(() if fresh else (out,)))


def fs_swap(value, step):
    return lax.ppermute(value, "fs", [(i, i ^ step) for i in range(lax.axis_size("fs"))])


def tp_swap(value, step):
    return lax.ppermute(value, "tp", [(i, i ^ step) for i in range(lax.axis_size("tp"))])


def plan(ways):
    pair = [(False, step) for step in range(ways)]
    far = [step for step in range(ways) if step >= ways // 2]
    near = [step for step in range(ways) if 0 < step < ways // 2]
    down = [(True, step) for step in far + near[1:] + near[:1] + [0]]
    return pair + down


def exchange_shards(
    prompt, norm_gain, gate_master, up_master, down_master, group_choice, inner_choice, route_weight
):
    ways = lax.axis_size("fs")
    mine, me = lax.axis_index("fs").astype(jnp.int32), lax.axis_index("tp").astype(jnp.int32)
    experts, rows, hidden = gate_master.shape
    held, total = experts // ways, rows * ways
    gain = jnp.broadcast_to(norm_gain[:, None], (rows, hidden))
    pieces = plan(ways)

    own, left, right, last = ({}, {}, {}, {})
    for index, (down, step) in enumerate(pieces):
        block = mine ^ step
        if down:
            cut = lax.dynamic_slice_in_dim(down_master, block * held, held, 0)
            piece = cut.astype(jnp.bfloat16)
        else:
            piece = cast_pair(block, gain, gate_master, up_master, held)
        if step:
            piece = fs_swap(piece, step)
        own[index] = piece
        left[index] = tp_swap(piece, 1)
        right[index] = tp_swap(piece, 2)
        last[index] = tp_swap(left[index], 2) if index % 2 == 0 else tp_swap(right[index], 1)

    def parts(index):
        return own[index], left[index], right[index], last[index]

    pair_out, down_out, scaled, sums = None, None, None, []
    for index, (down, step) in enumerate(pieces):
        where = jnp.stack([mine ^ step, me])
        if not down:
            pair_out = lay_pair(where, parts(index), pair_out, total)
            continue
        if scaled is None:
            gate_local, up_local = pair_out
            column_weight = route_columns(
                group_choice, inner_choice, route_weight, gate_local.shape[1]
            )
            scaled = activations(normalize(prompt), gate_local, up_local, column_weight)
        down_out, partial = lay_down(where, parts(index), scaled, down_out, total)
        if step:
            partial = fs_swap(partial, step)
        sums.append(partial)
    mixed = (sum(sums[1:], sums[0]) * FF ** (-0.5)).astype(jnp.bfloat16)
    return (*pair_out, down_out, mixed)


def solution(mesh):
    in_specs = (
        P("tp", None),
        P("fs"),
        P(None, "fs", "tp"),
        P(None, "fs", "tp"),
        P(None, "fs", "tp"),
        P("tp"),
        P("tp", None),
        P("tp", None),
    )
    out_specs = (P(None, "fs"), P(None, "fs"), P(None, "fs"), P("tp", "fs"))
    wrap = functools.partial(
        jax.shard_map, mesh=mesh, in_specs=in_specs, out_specs=out_specs, check_vma=False
    )
    ways, parts = mesh.shape["fs"], mesh.shape["tp"]
    whole_experts = ways & (ways - 1) == 0 and ways >= 4 and (GROUPS * EPG) % ways == 0
    if not (whole_experts and parts == 4 and FF % (parts * LANES) == 0):
        return wrap(general_shards)

    return wrap(exchange_shards)
```

```python
import functools

import jax
import jax.numpy as jnp
from jax import lax
from jax.experimental import pallas as pl
from jax.experimental.pallas import tpu as pltpu
from jax.sharding import PartitionSpec as P

FF = 512
GROUPS = 4
EPG = 8
LANES = 128
HERE = (0, 0)
ANYWHERE = pl.BlockSpec(memory_space=pl.ANY)
ROOM = pltpu.CompilerParams(vmem_limit_bytes=63 * 2**20)


def flatten_rows(piece):
    count, experts, rows, hidden = piece.shape
    return piece.transpose(0, 2, 1, 3).reshape(count, rows, experts * hidden)


def restore_rows(gathered, rows):
    parts = lax.axis_size("tp")
    count, total, width = gathered.shape
    blocks = total // (parts * rows)
    ordered = gathered.reshape(count, parts, blocks, rows, width).transpose(0, 2, 1, 3, 4)
    return ordered.reshape(count, total, width)


def activations(normed, gate_local, up_local, column_weight):
    width = normed.shape[1]
    gate_act = jnp.dot(normed, gate_local, preferred_element_type=jnp.float32) * width ** (-0.5)
    up_act = jnp.dot(normed, up_local, preferred_element_type=jnp.float32) * width ** (-0.5)
    return (column_weight * jax.nn.silu(gate_act) * up_act).astype(jnp.bfloat16)


def route_columns(group_choice, inner_choice, route_weight, columns):
    first = lax.axis_index("fs") * columns
    owner = (first + jnp.arange(columns, dtype=jnp.int32)) // FF
    chosen = group_choice[:, None] * EPG + inner_choice
    picked = jnp.where(chosen[:, :, None] == owner[None, None, :], route_weight[:, :, None], 0.0)
    return jnp.sum(picked, axis=1)


def normalize(prompt):
    values = prompt.astype(jnp.float32)
    mean = jnp.mean(values * values, axis=1, keepdims=True)
    return (values * lax.rsqrt(mean + 1e-06)).astype(jnp.bfloat16)


def general_shards(
    prompt, norm_gain, gate_master, up_master, down_master, group_choice, inner_choice, route_weight
):
    scale = norm_gain[None, :, None]
    gate_cast = (gate_master * scale).astype(jnp.bfloat16)
    up_cast = (up_master * scale).astype(jnp.bfloat16)
    down_cast = down_master.astype(jnp.bfloat16)
    rows = gate_master.shape[1] // lax.axis_size("tp")
    normed = normalize(prompt)
    stacked = jnp.stack([gate_cast, up_cast, down_cast])
    widened = lax.all_to_all(stacked, "tp", split_axis=2, concat_axis=3, tiled=True)
    moved = lax.all_to_all(flatten_rows(widened), "fs", split_axis=2, concat_axis=1, tiled=True)
    served = restore_rows(lax.all_gather(moved, "tp", axis=1, tiled=True), rows)
    gate_local, up_local, down_local = (served[0], served[1], served[2])
    column_weight = route_columns(group_choice, inner_choice, route_weight, gate_local.shape[1])
    scaled = activations(normed, gate_local, up_local, column_weight)
    summed = lax.psum_scatter(
        lax.dot_general(
            down_local, scaled, (((1,), (1,)), ((), ())), preferred_element_type=jnp.float32
        ),
        "fs",
        scatter_dimension=0,
        tiled=True,
    )
    mixed = (summed * FF ** (-0.5)).T.astype(jnp.bfloat16)
    return (gate_local, up_local, down_local, mixed)


def partner(index, offset, ways, sign):
    chips, core = offset
    chip = lax.rem(index // 2 + (chips if sign > 0 else ways // 2 - chips), ways // 2)
    return chip * 2 + (index % 2 if core == 0 else 1 - index % 2)


def receiver(offset):
    return partner(lax.axis_index("fs"), offset, lax.axis_size("fs"), 1)


def sender(offset):
    return partner(lax.axis_index("fs"), offset, lax.axis_size("fs"), -1)


def cast_kernel(steps, gain_ref, gate_ref, up_ref, *refs):
    outs, (gate_buf, up_buf, out_buf, in_sem, out_sem) = refs[: len(steps)], refs[len(steps) :]
    held, rows, hidden = gate_buf.shape[1:]
    loads, stores = [], []
    for i, step in enumerate(steps):
        experts = pl.ds(receiver(step) * held, held)
        pair = [
            pltpu.make_async_copy(gate_ref.at[experts], gate_buf.at[i], in_sem.at[i, 0]),
            pltpu.make_async_copy(up_ref.at[experts], up_buf.at[i], in_sem.at[i, 1]),
        ]
        for copy in pair:
            copy.start()
        loads.append(pair)
    gain = jnp.broadcast_to(gain_ref[...], (hidden, rows)).T
    for i, out in enumerate(outs):
        for which, source in enumerate((gate_buf, up_buf)):
            loads[i][which].wait()
            for e in range(held):
                out_buf[i, which, e] = (source[i, e] * gain).astype(jnp.bfloat16)
        stores.append(pltpu.make_async_copy(out_buf.at[i], out, out_sem.at[i]))
        stores[i].start()
    for copy in stores:
        copy.wait()


def cast_pairs(steps, norm_gain, gate_master, up_master, held):
    _, rows, hidden = gate_master.shape
    count = len(steps)
    piece = jax.ShapeDtypeStruct((2, held, rows, hidden), jnp.bfloat16)
    return pl.pallas_call(
        functools.partial(cast_kernel, steps),
        in_specs=[pl.BlockSpec(memory_space=pltpu.VMEM), ANYWHERE, ANYWHERE],
        out_specs=[ANYWHERE] * count,
        out_shape=[piece] * count,
        scratch_shapes=[
            pltpu.VMEM((count, held, rows, hidden), jnp.float32),
            pltpu.VMEM((count, held, rows, hidden), jnp.float32),
            pltpu.VMEM((count, *piece.shape), jnp.bfloat16),
            pltpu.SemaphoreType.DMA((count, 2)),
            pltpu.SemaphoreType.DMA((count,)),
        ],
        compiler_params=ROOM,
    )(norm_gain[None, :], gate_master, up_master)


def column_of(expert, swap, hidden):
    return pl.multiple_of((expert * 4 + (lax.axis_index("tp") ^ swap)) * hidden, LANES)


def lay_pair_kernel(step, *refs):
    parts, (gate_out, up_out, held_buf, in_sem, out_sem) = refs[:4], refs[-5:]
    _, held, rows, hidden = parts[0].shape
    first = pl.multiple_of(sender(step) * rows, LANES)
    loads, stores = [], []
    for which in range(2):
        for swap, part in enumerate(parts):
            loads.append(
                pltpu.make_async_copy(
                    part.at[which], held_buf.at[which, swap], in_sem.at[which, swap]
                )
            )
            loads[-1].start()
    for which, out in enumerate((gate_out, up_out)):
        for swap in range(4):
            loads[which * 4 + swap].wait()
            for e in range(held):
                place = out.at[pl.ds(first, rows), pl.ds(column_of(e, swap, hidden), hidden)]
                stores.append(
                    pltpu.make_async_copy(
                        held_buf.at[which, swap, e], place, out_sem.at[which, swap, e]
                    )
                )
                stores[-1].start()
    for copy in stores:
        copy.wait()


def lay_pair(step, parts, outs, total):
    _, held, rows, hidden = parts[0].shape
    fresh = outs is None
    shape = jax.ShapeDtypeStruct((total, held * 4 * hidden), jnp.bfloat16)
    return pl.pallas_call(
        functools.partial(lay_pair_kernel, step),
        in_specs=[ANYWHERE] * (4 if fresh else 6),
        out_specs=[ANYWHERE, ANYWHERE],
        out_shape=[shape, shape],
        scratch_shapes=[
            pltpu.VMEM((2, 4, held, rows, hidden), jnp.bfloat16),
            pltpu.SemaphoreType.DMA((2, 4)),
            pltpu.SemaphoreType.DMA((2, 4, held)),
        ],
        input_output_aliases={} if fresh else {4: 0, 5: 1},
        compiler_params=ROOM,
    )(*parts, *(() if fresh else outs))


def lay_down_kernel(step, sums, factor, *refs):
    parts, scaled_ref, others = refs[:4], refs[4], refs[5 : 5 + sums]
    out, result_ref, held_buf, block, scaled_buf, sum_buf, in_sem, sum_sem, sems = refs[-9:]
    held, rows, hidden = parts[0].shape
    first = pl.multiple_of(sender(step) * rows, LANES)
    loads = [
        pltpu.make_async_copy(part, held_buf.at[swap], in_sem.at[swap])
        for swap, part in enumerate(parts)
    ]
    loads.append(pltpu.make_async_copy(scaled_ref, scaled_buf, sems.at[0]))
    for i, other in enumerate(others):
        loads.append(pltpu.make_async_copy(other, sum_buf.at[i], sum_sem.at[i]))
    for copy in loads:
        copy.start()
    for swap in range(4):
        loads[swap].wait()
        for e in range(held):
            block[:, pl.ds(column_of(e, swap, hidden), hidden)] = held_buf[swap, e]
    store = pltpu.make_async_copy(block, out.at[pl.ds(first, rows), :], sems.at[1])
    store.start()
    loads[4].wait()
    product = lax.dot_general(
        scaled_buf[...], block[...], (((1,), (1,)), ((), ())), preferred_element_type=jnp.float32
    )
    if sums:
        for i in range(sums):
            loads[5 + i].wait()
            product += sum_buf[i].astype(jnp.float32)
        product *= factor
    result_ref[...] = product.astype(result_ref.dtype)
    store.wait()


def lay_down(step, parts, scaled, others, out, total):
    held, rows, hidden = parts[0].shape
    width = held * 4 * hidden
    tokens = scaled.shape[0]
    fresh = out is None
    sums = len(others)
    return pl.pallas_call(
        functools.partial(lay_down_kernel, step, sums, FF ** (-0.5)),
        in_specs=[ANYWHERE] * (5 + sums + (0 if fresh else 1)),
        out_specs=[ANYWHERE, pl.BlockSpec(memory_space=pltpu.VMEM)],
        out_shape=[
            jax.ShapeDtypeStruct((total, width), jnp.bfloat16),
            jax.ShapeDtypeStruct((tokens, rows), jnp.bfloat16),
        ],
        scratch_shapes=[
            pltpu.VMEM((4, held, rows, hidden), jnp.bfloat16),
            pltpu.VMEM((rows, width), jnp.bfloat16),
            pltpu.VMEM((tokens, width), jnp.bfloat16),
            pltpu.VMEM((max(sums, 1), tokens, rows), jnp.bfloat16),
            pltpu.SemaphoreType.DMA((4,)),
            pltpu.SemaphoreType.DMA((max(sums, 1),)),
            pltpu.SemaphoreType.DMA((2,)),
        ],
        input_output_aliases={} if fresh else {5 + sums: 0},
        compiler_params=ROOM,
    )(*parts, scaled, *others, *(() if fresh else (out,)))


def act_kernel(normed_ref, gate_ref, up_ref, chosen_ref, weight_ref, out_ref):
    owner = lax.axis_index("fs") * pl.num_programs(0) + pl.program_id(0)
    picked = jnp.where(chosen_ref[...] == owner, weight_ref[...], 0.0)
    weight = jnp.sum(picked, axis=1, keepdims=True)
    normed = normed_ref[...]
    factor = normed.shape[1] ** (-0.5)
    gate = jnp.dot(normed, gate_ref[...], preferred_element_type=jnp.float32) * factor
    up = jnp.dot(normed, up_ref[...], preferred_element_type=jnp.float32) * factor
    out_ref[...] = (weight * (gate / (1.0 + jnp.exp(-gate))) * up).astype(jnp.bfloat16)


def act(normed, gate_local, up_local, chosen, route_weight, held):
    tokens, width = normed.shape
    block = gate_local.shape[1] // held
    whole = lambda array: pl.BlockSpec(array.shape, lambda e: (0, 0))
    columns = pl.BlockSpec((width, block), lambda e: (0, e))
    return pl.pallas_call(
        act_kernel,
        grid=(held,),
        in_specs=[whole(normed), columns, columns, whole(chosen), whole(route_weight)],
        out_specs=pl.BlockSpec((tokens, block), lambda e: (0, e)),
        out_shape=jax.ShapeDtypeStruct((tokens, held * block), jnp.bfloat16),
        compiler_params=ROOM,
    )(normed, gate_local, up_local, chosen, route_weight)


def fs_send(value, offset, sign):
    ways = lax.axis_size("fs")
    chips = offset[0] if sign > 0 else ways // 2 - offset[0]
    pairs = [
        (i, (i // 2 + chips) % (ways // 2) * 2 + (i % 2 ^ offset[1])) for i in range(ways)
    ]
    return lax.ppermute(value, "fs", pairs)


def tp_swap(value, step):
    return lax.ppermute(value, "tp", [(i, i ^ step) for i in range(lax.axis_size("tp"))])


def plan(ways):
    chips = ways // 2
    apart = []
    for near in range(1, chips // 2 + 1):
        both = [near] if 2 * near == chips else [near, chips - near]
        apart += [(far, core) for core in range(2) for far in both]
    pair = [(False, offset) for offset in [(0, 0), (0, 1)] + apart]
    return pair + [(True, offset) for offset in apart + [(0, 1), (0, 0)]]


def turns(pieces):
    seen = {True: 0, False: 0}
    result = []
    for down, _ in pieces:
        result.append(seen[down] % 2 == 0)
        seen[down] += 1
    return result


def exchange_shards(
    prompt, norm_gain, gate_master, up_master, down_master, group_choice, inner_choice, route_weight
):
    ways = lax.axis_size("fs")
    experts, rows, _ = gate_master.shape
    held, total = experts // ways, rows * ways
    pieces = plan(ways)

    cast = cast_pairs((HERE,), norm_gain, gate_master, up_master, held)
    others = tuple(offset for down, offset in pieces[1:] if not down)
    cast += cast_pairs(others, norm_gain, gate_master, up_master, held)

    own, left, right, last = ({}, {}, {}, {})
    turn = turns(pieces)
    for index, (down, step) in enumerate(pieces):
        if down:
            cut = lax.dynamic_slice_in_dim(down_master, receiver(step) * held, held, 0)
            piece = cut.astype(jnp.bfloat16)
        else:
            piece = cast[index]
        if step != HERE:
            piece = fs_send(piece, step, 1)
        own[index] = piece
        left[index] = tp_swap(piece, 1)
        right[index] = tp_swap(piece, 2)
        last[index] = tp_swap(left[index], 2) if turn[index] else tp_swap(right[index], 1)

    pair_out, down_out, scaled, sums = None, None, None, ()
    for index, (down, step) in enumerate(pieces):
        parts = own[index], left[index], right[index], last[index]
        if not down:
            pair_out = lay_pair(step, parts, pair_out, total)
            continue
        if scaled is None:
            normed, chosen = normalize(prompt), group_choice[:, None] * EPG + inner_choice
            scaled = act(normed, *pair_out, chosen, route_weight, held)
        down_out, result = lay_down(
            step, parts, scaled, sums if step == HERE else (), down_out, total
        )
        if step != HERE:
            sums += (fs_send(result, step, -1),)
    return (*pair_out, down_out, result)


def solution(mesh):
    in_specs = (
        P("tp", None),
        P("fs"),
        P(None, "fs", "tp"),
        P(None, "fs", "tp"),
        P(None, "fs", "tp"),
        P("tp"),
        P("tp", None),
        P("tp", None),
    )
    out_specs = (P(None, "fs"), P(None, "fs"), P(None, "fs"), P("tp", "fs"))
    wrap = functools.partial(
        jax.shard_map, mesh=mesh, in_specs=in_specs, out_specs=out_specs, check_vma=False
    )
    ways, parts = mesh.shape["fs"], mesh.shape["tp"]
    whole_experts = ways & (ways - 1) == 0 and ways >= 4 and (GROUPS * EPG) % ways == 0
    if not (whole_experts and parts == 4 and FF % (parts * LANES) == 0):
        return wrap(general_shards)

    return wrap(exchange_shards)
```

```python
import functools

import jax
import jax.numpy as jnp
from jax import lax
from jax.experimental import pallas as pl
from jax.experimental.pallas import tpu as pltpu
from jax.sharding import PartitionSpec as P

FF = 512
GROUPS = 4
EPG = 8
LANES = 128
HERE = (0, 0)
ANYWHERE = pl.BlockSpec(memory_space=pl.ANY)
ROOM = pltpu.CompilerParams(vmem_limit_bytes=67_000_000)


def flatten_rows(piece):
    count, experts, rows, hidden = piece.shape
    return piece.transpose(0, 2, 1, 3).reshape(count, rows, experts * hidden)


def restore_rows(gathered, rows):
    parts = lax.axis_size("tp")
    count, total, width = gathered.shape
    blocks = total // (parts * rows)
    ordered = gathered.reshape(count, parts, blocks, rows, width).transpose(0, 2, 1, 3, 4)
    return ordered.reshape(count, total, width)


def activations(normed, gate_local, up_local, column_weight):
    width = normed.shape[1]
    gate_act = jnp.dot(normed, gate_local, preferred_element_type=jnp.float32) * width ** (-0.5)
    up_act = jnp.dot(normed, up_local, preferred_element_type=jnp.float32) * width ** (-0.5)
    return (column_weight * jax.nn.silu(gate_act) * up_act).astype(jnp.bfloat16)


def route_columns(group_choice, inner_choice, route_weight, columns):
    first = lax.axis_index("fs") * columns
    owner = (first + jnp.arange(columns, dtype=jnp.int32)) // FF
    chosen = group_choice[:, None] * EPG + inner_choice
    picked = jnp.where(chosen[:, :, None] == owner[None, None, :], route_weight[:, :, None], 0.0)
    return jnp.sum(picked, axis=1)


def normalize(prompt):
    values = prompt.astype(jnp.float32)
    mean = jnp.mean(values * values, axis=1, keepdims=True)
    return (values * lax.rsqrt(mean + 1e-06)).astype(jnp.bfloat16)


def general_shards(
    prompt, norm_gain, gate_master, up_master, down_master, group_choice, inner_choice, route_weight
):
    scale = norm_gain[None, :, None]
    gate_cast = (gate_master * scale).astype(jnp.bfloat16)
    up_cast = (up_master * scale).astype(jnp.bfloat16)
    down_cast = down_master.astype(jnp.bfloat16)
    rows = gate_master.shape[1] // lax.axis_size("tp")
    normed = normalize(prompt)
    stacked = jnp.stack([gate_cast, up_cast, down_cast])
    widened = lax.all_to_all(stacked, "tp", split_axis=2, concat_axis=3, tiled=True)
    moved = lax.all_to_all(flatten_rows(widened), "fs", split_axis=2, concat_axis=1, tiled=True)
    served = restore_rows(lax.all_gather(moved, "tp", axis=1, tiled=True), rows)
    gate_local, up_local, down_local = (served[0], served[1], served[2])
    column_weight = route_columns(group_choice, inner_choice, route_weight, gate_local.shape[1])
    scaled = activations(normed, gate_local, up_local, column_weight)
    summed = lax.psum_scatter(
        lax.dot_general(
            down_local, scaled, (((1,), (1,)), ((), ())), preferred_element_type=jnp.float32
        ),
        "fs",
        scatter_dimension=0,
        tiled=True,
    )
    mixed = (summed * FF ** (-0.5)).T.astype(jnp.bfloat16)
    return (gate_local, up_local, down_local, mixed)


def partner(index, offset, ways, sign):
    chips, core = offset
    chip = lax.rem(index // 2 + (chips if sign > 0 else ways // 2 - chips), ways // 2)
    return chip * 2 + (index % 2 if core == 0 else 1 - index % 2)


def receiver(offset):
    return partner(lax.axis_index("fs"), offset, lax.axis_size("fs"), 1)


def sender(offset):
    return partner(lax.axis_index("fs"), offset, lax.axis_size("fs"), -1)


def cast_kernel(steps, gain_ref, gate_ref, up_ref, *refs):
    outs, (gate_buf, up_buf, out_buf, in_sem, out_sem) = refs[: len(steps)], refs[len(steps) :]
    held, rows, hidden = gate_buf.shape[1:]
    loads, stores = [], []
    for i, step in enumerate(steps):
        experts = pl.ds(receiver(step) * held, held)
        pair = [
            pltpu.make_async_copy(gate_ref.at[experts], gate_buf.at[i], in_sem.at[i, 0]),
            pltpu.make_async_copy(up_ref.at[experts], up_buf.at[i], in_sem.at[i, 1]),
        ]
        for copy in pair:
            copy.start()
        loads.append(pair)
    gain = jnp.broadcast_to(gain_ref[...], (hidden, rows)).T
    for i, out in enumerate(outs):
        for which, source in enumerate((gate_buf, up_buf)):
            loads[i][which].wait()
            for e in range(held):
                out_buf[i, which, e] = (source[i, e] * gain).astype(jnp.bfloat16)
        stores.append(pltpu.make_async_copy(out_buf.at[i], out, out_sem.at[i]))
        stores[i].start()
    for copy in stores:
        copy.wait()


def cast_pairs(steps, norm_gain, gate_master, up_master, held):
    _, rows, hidden = gate_master.shape
    count = len(steps)
    piece = jax.ShapeDtypeStruct((2, held, rows, hidden), jnp.bfloat16)
    return pl.pallas_call(
        functools.partial(cast_kernel, steps),
        in_specs=[pl.BlockSpec(memory_space=pltpu.VMEM), ANYWHERE, ANYWHERE],
        out_specs=[ANYWHERE] * count,
        out_shape=[piece] * count,
        scratch_shapes=[
            pltpu.VMEM((count, held, rows, hidden), jnp.float32),
            pltpu.VMEM((count, held, rows, hidden), jnp.float32),
            pltpu.VMEM((count, *piece.shape), jnp.bfloat16),
            pltpu.SemaphoreType.DMA((count, 2)),
            pltpu.SemaphoreType.DMA((count,)),
        ],
        compiler_params=ROOM,
    )(norm_gain[None, :], gate_master, up_master)


def cast_down_kernel(steps, down_ref, *refs):
    outs, (down_buf, out_buf, in_sem, out_sem) = refs[: len(steps)], refs[len(steps) :]
    held = down_buf.shape[1]
    loads, stores = [], []
    for i, step in enumerate(steps):
        experts = pl.ds(receiver(step) * held, held)
        loads.append(pltpu.make_async_copy(down_ref.at[experts], down_buf.at[i], in_sem.at[i]))
        loads[i].start()
    for i, out in enumerate(outs):
        loads[i].wait()
        for e in range(held):
            out_buf[i, e] = down_buf[i, e].astype(jnp.bfloat16)
        stores.append(pltpu.make_async_copy(out_buf.at[i], out, out_sem.at[i]))
        stores[i].start()
    for copy in stores:
        copy.wait()


def cast_down(steps, down_master, held):
    _, rows, hidden = down_master.shape
    count = len(steps)
    piece = jax.ShapeDtypeStruct((held, rows, hidden), jnp.bfloat16)
    return pl.pallas_call(
        functools.partial(cast_down_kernel, steps),
        in_specs=[ANYWHERE],
        out_specs=[ANYWHERE] * count,
        out_shape=[piece] * count,
        scratch_shapes=[
            pltpu.VMEM((count, *piece.shape), jnp.float32),
            pltpu.VMEM((count, *piece.shape), jnp.bfloat16),
            pltpu.SemaphoreType.DMA((count,)),
            pltpu.SemaphoreType.DMA((count,)),
        ],
        compiler_params=ROOM,
    )(down_master)


def column_of(expert, swap, hidden):
    return pl.multiple_of((expert * 4 + (lax.axis_index("tp") ^ swap)) * hidden, LANES)


def lay_pair_kernel(step, *refs):
    parts, (gate_out, up_out, held_buf, in_sem, out_sem) = refs[:4], refs[-5:]
    _, held, rows, hidden = parts[0].shape
    first = pl.multiple_of(sender(step) * rows, LANES)
    loads, stores = [], []
    for which in range(2):
        for swap, part in enumerate(parts):
            loads.append(
                pltpu.make_async_copy(
                    part.at[which], held_buf.at[which, swap], in_sem.at[which, swap]
                )
            )
            loads[-1].start()
    for which, out in enumerate((gate_out, up_out)):
        for swap in range(4):
            loads[which * 4 + swap].wait()
            for e in range(held):
                place = out.at[pl.ds(first, rows), pl.ds(column_of(e, swap, hidden), hidden)]
                stores.append(
                    pltpu.make_async_copy(
                        held_buf.at[which, swap, e], place, out_sem.at[which, swap, e]
                    )
                )
                stores[-1].start()
    for copy in stores:
        copy.wait()


def lay_pair(step, parts, outs, total):
    _, held, rows, hidden = parts[0].shape
    fresh = outs is None
    shape = jax.ShapeDtypeStruct((total, held * 4 * hidden), jnp.bfloat16)
    return pl.pallas_call(
        functools.partial(lay_pair_kernel, step),
        in_specs=[ANYWHERE] * (4 if fresh else 6),
        out_specs=[ANYWHERE, ANYWHERE],
        out_shape=[shape, shape],
        scratch_shapes=[
            pltpu.VMEM((2, 4, held, rows, hidden), jnp.bfloat16),
            pltpu.SemaphoreType.DMA((2, 4)),
            pltpu.SemaphoreType.DMA((2, 4, held)),
        ],
        input_output_aliases={} if fresh else {4: 0, 5: 1},
        compiler_params=ROOM,
    )(*parts, *(() if fresh else outs))


def lay_down_kernel(step, sums, factor, *refs):
    parts, scaled_ref, others = refs[:4], refs[4], refs[5 : 5 + sums]
    out, result_ref, held_buf, block, scaled_buf, sum_buf, in_sem, sum_sem, sems = refs[-9:]
    held, rows, hidden = parts[0].shape
    first = pl.multiple_of(sender(step) * rows, LANES)
    loads = [
        pltpu.make_async_copy(part, held_buf.at[swap], in_sem.at[swap])
        for swap, part in enumerate(parts)
    ]
    loads.append(pltpu.make_async_copy(scaled_ref, scaled_buf, sems.at[0]))
    for i, other in enumerate(others):
        loads.append(pltpu.make_async_copy(other, sum_buf.at[i], sum_sem.at[i]))
    for copy in loads:
        copy.start()
    for swap in range(4):
        loads[swap].wait()
        for e in range(held):
            block[:, pl.ds(column_of(e, swap, hidden), hidden)] = held_buf[swap, e]
    store = pltpu.make_async_copy(block, out.at[pl.ds(first, rows), :], sems.at[1])
    store.start()
    loads[4].wait()
    product = lax.dot_general(
        scaled_buf[...], block[...], (((1,), (1,)), ((), ())), preferred_element_type=jnp.float32
    )
    if sums:
        for i in range(sums):
            loads[5 + i].wait()
            product += sum_buf[i].astype(jnp.float32)
        product *= factor
    result_ref[...] = product.astype(result_ref.dtype)
    store.wait()


def lay_down(step, parts, scaled, others, out, total):
    held, rows, hidden = parts[0].shape
    width = held * 4 * hidden
    tokens = scaled.shape[0]
    fresh = out is None
    sums = len(others)
    return pl.pallas_call(
        functools.partial(lay_down_kernel, step, sums, FF ** (-0.5)),
        in_specs=[ANYWHERE] * (5 + sums + (0 if fresh else 1)),
        out_specs=[ANYWHERE, pl.BlockSpec(memory_space=pltpu.VMEM)],
        out_shape=[
            jax.ShapeDtypeStruct((total, width), jnp.bfloat16),
            jax.ShapeDtypeStruct((tokens, rows), jnp.bfloat16),
        ],
        scratch_shapes=[
            pltpu.VMEM((4, held, rows, hidden), jnp.bfloat16),
            pltpu.VMEM((rows, width), jnp.bfloat16),
            pltpu.VMEM((tokens, width), jnp.bfloat16),
            pltpu.VMEM((max(sums, 1), tokens, rows), jnp.bfloat16),
            pltpu.SemaphoreType.DMA((4,)),
            pltpu.SemaphoreType.DMA((max(sums, 1),)),
            pltpu.SemaphoreType.DMA((2,)),
        ],
        input_output_aliases={} if fresh else {5 + sums: 0},
        compiler_params=ROOM,
    )(*parts, scaled, *others, *(() if fresh else (out,)))


def ready_kernel(held, prompt_ref, group_ref, inner_ref, route_ref, normed_ref, weight_ref):
    values = prompt_ref[...].astype(jnp.float32)
    mean = jnp.mean(values * values, axis=1, keepdims=True)
    normed_ref[...] = (values * lax.rsqrt(mean + 1e-06)).astype(jnp.bfloat16)
    chosen = group_ref[...] * EPG + inner_ref[...]
    for e in range(held):
        owner = lax.axis_index("fs") * held + e
        picked = jnp.where(chosen == owner, route_ref[...], 0.0)
        row = jnp.sum(picked, axis=0, keepdims=True)
        weight_ref[e] = jnp.broadcast_to(row, (LANES, row.shape[1])).T


def ready(prompt, group_choice, inner_choice, route_weight, held):
    tokens = prompt.shape[0]
    near = pl.BlockSpec(memory_space=pltpu.VMEM)
    return pl.pallas_call(
        functools.partial(ready_kernel, held),
        in_specs=[near] * 4,
        out_specs=[near] * 2,
        out_shape=[
            jax.ShapeDtypeStruct(prompt.shape, jnp.bfloat16),
            jax.ShapeDtypeStruct((held, tokens, LANES), jnp.float32),
        ],
        compiler_params=ROOM,
    )(prompt, group_choice[None, :], inner_choice.T, route_weight.T)


def act_kernel(normed_ref, gate_ref, up_ref, weight_ref, out_ref):
    normed = normed_ref[...]
    factor = normed.shape[1] ** (-0.5)
    gate = jnp.dot(normed, gate_ref[...], preferred_element_type=jnp.float32) * factor
    up = jnp.dot(normed, up_ref[...], preferred_element_type=jnp.float32) * factor
    weight = jnp.concatenate([weight_ref[0]] * (gate.shape[1] // LANES), axis=1)
    out_ref[...] = (weight * (gate / (1.0 + jnp.exp(-gate))) * up).astype(jnp.bfloat16)


def act(normed, gate_local, up_local, weight):
    tokens, width = normed.shape
    held = weight.shape[0]
    block = gate_local.shape[1] // held
    columns = pl.BlockSpec((width, block), lambda e: (0, e))
    return pl.pallas_call(
        act_kernel,
        grid=(held,),
        in_specs=[
            pl.BlockSpec(normed.shape, lambda e: (0, 0)),
            columns,
            columns,
            pl.BlockSpec((1, tokens, LANES), lambda e: (e, 0, 0)),
        ],
        out_specs=pl.BlockSpec((tokens, block), lambda e: (0, e)),
        out_shape=jax.ShapeDtypeStruct((tokens, held * block), jnp.bfloat16),
        compiler_params=ROOM,
    )(normed, gate_local, up_local, weight)


def fs_send(value, offset, sign):
    ways = lax.axis_size("fs")
    chips = offset[0] if sign > 0 else ways // 2 - offset[0]
    pairs = [
        (i, (i // 2 + chips) % (ways // 2) * 2 + (i % 2 ^ offset[1])) for i in range(ways)
    ]
    return lax.ppermute(value, "fs", pairs)


def tp_swap(value, step):
    return lax.ppermute(value, "tp", [(i, i ^ step) for i in range(lax.axis_size("tp"))])


def plan(ways):
    chips = ways // 2
    apart = []
    for near in range(1, chips // 2 + 1):
        both = [near] if 2 * near == chips else [near, chips - near]
        apart += [(far, core) for core in range(2) for far in both]
    pair = [(False, offset) for offset in [(0, 0), (0, 1)] + apart]
    apart.sort(key=lambda offset: -min(offset[0], chips - offset[0]))
    return pair + [(True, offset) for offset in apart + [(0, 1), (0, 0)]]


def turns(pieces):
    seen = {True: 0, False: 0}
    result = []
    for down, _ in pieces:
        result.append(seen[down] % 2 == 0)
        seen[down] += 1
    return result


def exchange_shards(
    prompt, norm_gain, gate_master, up_master, down_master, group_choice, inner_choice, route_weight
):
    ways = lax.axis_size("fs")
    experts, rows, _ = gate_master.shape
    held, total = experts // ways, rows * ways
    pieces = plan(ways)

    cast = cast_pairs((HERE,), norm_gain, gate_master, up_master, held)
    others = tuple(offset for down, offset in pieces[1:] if not down)
    cast += cast_pairs(others, norm_gain, gate_master, up_master, held)
    normed, weight = ready(prompt, group_choice, inner_choice, route_weight, held)
    cast += cast_down(tuple(offset for down, offset in pieces if down), down_master, held)

    own, left, right, last = ({}, {}, {}, {})
    turn = turns(pieces)
    for index, (down, step) in enumerate(pieces):
        piece = cast[index]
        if step != HERE:
            piece = fs_send(piece, step, 1)
        own[index] = piece
        left[index] = tp_swap(piece, 1)
        right[index] = tp_swap(piece, 2)
        last[index] = tp_swap(left[index], 2) if turn[index] else tp_swap(right[index], 1)

    pair_out, down_out, scaled, sums = None, None, None, ()
    for index, (down, step) in enumerate(pieces):
        parts = own[index], left[index], right[index], last[index]
        if not down:
            pair_out = lay_pair(step, parts, pair_out, total)
            continue
        if scaled is None:
            scaled = act(normed, *pair_out, weight)
        down_out, result = lay_down(
            step, parts, scaled, sums if step == HERE else (), down_out, total
        )
        if step != HERE:
            sums += (fs_send(result, step, -1),)
    return (*pair_out, down_out, result)


def solution(mesh):
    in_specs = (
        P("tp", None),
        P("fs"),
        P(None, "fs", "tp"),
        P(None, "fs", "tp"),
        P(None, "fs", "tp"),
        P("tp"),
        P("tp", None),
        P("tp", None),
    )
    out_specs = (P(None, "fs"), P(None, "fs"), P(None, "fs"), P("tp", "fs"))
    wrap = functools.partial(
        jax.shard_map, mesh=mesh, in_specs=in_specs, out_specs=out_specs, check_vma=False
    )
    ways, parts = mesh.shape["fs"], mesh.shape["tp"]
    whole_experts = ways & (ways - 1) == 0 and ways >= 4 and (GROUPS * EPG) % ways == 0
    if not (whole_experts and parts == 4 and FF % (parts * LANES) == 0):
        return wrap(general_shards)

    return wrap(exchange_shards)
```

```python
import functools

import jax
import jax.numpy as jnp
from jax import lax
from jax.experimental import pallas as pl
from jax.experimental.pallas import tpu as pltpu
from jax.sharding import PartitionSpec as P

FF = 512
GROUPS = 4
EPG = 8
LANES = 128
HERE = (0, 0)
ANYWHERE = pl.BlockSpec(memory_space=pl.ANY)
ROOM = pltpu.CompilerParams(vmem_limit_bytes=67_000_000)


def flatten_rows(piece):
    count, experts, rows, hidden = piece.shape
    return piece.transpose(0, 2, 1, 3).reshape(count, rows, experts * hidden)


def restore_rows(gathered, rows):
    parts = lax.axis_size("tp")
    count, total, width = gathered.shape
    blocks = total // (parts * rows)
    ordered = gathered.reshape(count, parts, blocks, rows, width).transpose(0, 2, 1, 3, 4)
    return ordered.reshape(count, total, width)


def activations(normed, gate_local, up_local, column_weight):
    width = normed.shape[1]
    gate_act = jnp.dot(normed, gate_local, preferred_element_type=jnp.float32) * width ** (-0.5)
    up_act = jnp.dot(normed, up_local, preferred_element_type=jnp.float32) * width ** (-0.5)
    return (column_weight * jax.nn.silu(gate_act) * up_act).astype(jnp.bfloat16)


def route_columns(group_choice, inner_choice, route_weight, columns):
    first = lax.axis_index("fs") * columns
    owner = (first + jnp.arange(columns, dtype=jnp.int32)) // FF
    chosen = group_choice[:, None] * EPG + inner_choice
    picked = jnp.where(chosen[:, :, None] == owner[None, None, :], route_weight[:, :, None], 0.0)
    return jnp.sum(picked, axis=1)


def normalize(prompt):
    values = prompt.astype(jnp.float32)
    mean = jnp.mean(values * values, axis=1, keepdims=True)
    return (values * lax.rsqrt(mean + 1e-06)).astype(jnp.bfloat16)


def general_shards(
    prompt, norm_gain, gate_master, up_master, down_master, group_choice, inner_choice, route_weight
):
    scale = norm_gain[None, :, None]
    gate_cast = (gate_master * scale).astype(jnp.bfloat16)
    up_cast = (up_master * scale).astype(jnp.bfloat16)
    down_cast = down_master.astype(jnp.bfloat16)
    rows = gate_master.shape[1] // lax.axis_size("tp")
    normed = normalize(prompt)
    stacked = jnp.stack([gate_cast, up_cast, down_cast])
    widened = lax.all_to_all(stacked, "tp", split_axis=2, concat_axis=3, tiled=True)
    moved = lax.all_to_all(flatten_rows(widened), "fs", split_axis=2, concat_axis=1, tiled=True)
    served = restore_rows(lax.all_gather(moved, "tp", axis=1, tiled=True), rows)
    gate_local, up_local, down_local = (served[0], served[1], served[2])
    column_weight = route_columns(group_choice, inner_choice, route_weight, gate_local.shape[1])
    scaled = activations(normed, gate_local, up_local, column_weight)
    summed = lax.psum_scatter(
        lax.dot_general(
            down_local, scaled, (((1,), (1,)), ((), ())), preferred_element_type=jnp.float32
        ),
        "fs",
        scatter_dimension=0,
        tiled=True,
    )
    mixed = (summed * FF ** (-0.5)).T.astype(jnp.bfloat16)
    return (gate_local, up_local, down_local, mixed)


def partner(index, offset, ways, sign):
    chips, core = offset
    chip = lax.rem(index // 2 + (chips if sign > 0 else ways // 2 - chips), ways // 2)
    return chip * 2 + (index % 2 if core == 0 else 1 - index % 2)


def receiver(offset):
    return partner(lax.axis_index("fs"), offset, lax.axis_size("fs"), 1)


def sender(offset):
    return partner(lax.axis_index("fs"), offset, lax.axis_size("fs"), -1)


def cast_kernel(steps, gain_ref, gate_ref, up_ref, *refs):
    outs, (gate_buf, up_buf, out_buf, in_sem, out_sem) = refs[: len(steps)], refs[len(steps) :]
    held, rows, hidden = gate_buf.shape[1:]
    loads, stores = [], []
    for i, step in enumerate(steps):
        experts = pl.ds(receiver(step) * held, held)
        pair = [
            pltpu.make_async_copy(gate_ref.at[experts], gate_buf.at[i], in_sem.at[i, 0]),
            pltpu.make_async_copy(up_ref.at[experts], up_buf.at[i], in_sem.at[i, 1]),
        ]
        for copy in pair:
            copy.start()
        loads.append(pair)
    gain = jnp.broadcast_to(gain_ref[...], (hidden, rows)).T
    for i, out in enumerate(outs):
        for which, source in enumerate((gate_buf, up_buf)):
            loads[i][which].wait()
            for e in range(held):
                out_buf[i, which, e] = (source[i, e] * gain).astype(jnp.bfloat16)
        stores.append(pltpu.make_async_copy(out_buf.at[i], out, out_sem.at[i]))
        stores[i].start()
    for copy in stores:
        copy.wait()


def cast_pairs(steps, norm_gain, gate_master, up_master, held):
    _, rows, hidden = gate_master.shape
    count = len(steps)
    piece = jax.ShapeDtypeStruct((2, held, rows, hidden), jnp.bfloat16)
    return pl.pallas_call(
        functools.partial(cast_kernel, steps),
        in_specs=[pl.BlockSpec(memory_space=pltpu.VMEM), ANYWHERE, ANYWHERE],
        out_specs=[ANYWHERE] * count,
        out_shape=[piece] * count,
        scratch_shapes=[
            pltpu.VMEM((count, held, rows, hidden), jnp.float32),
            pltpu.VMEM((count, held, rows, hidden), jnp.float32),
            pltpu.VMEM((count, *piece.shape), jnp.bfloat16),
            pltpu.SemaphoreType.DMA((count, 2)),
            pltpu.SemaphoreType.DMA((count,)),
        ],
        compiler_params=ROOM,
    )(norm_gain[None, :], gate_master, up_master)


def cast_down_kernel(steps, down_ref, *refs):
    outs, (down_buf, out_buf, in_sem, out_sem) = refs[: len(steps)], refs[len(steps) :]
    held = down_buf.shape[1]
    loads, stores = [], []
    for i, step in enumerate(steps):
        experts = pl.ds(receiver(step) * held, held)
        loads.append(pltpu.make_async_copy(down_ref.at[experts], down_buf.at[i], in_sem.at[i]))
        loads[i].start()
    for i, out in enumerate(outs):
        loads[i].wait()
        for e in range(held):
            out_buf[i, e] = down_buf[i, e].astype(jnp.bfloat16)
        stores.append(pltpu.make_async_copy(out_buf.at[i], out, out_sem.at[i]))
        stores[i].start()
    for copy in stores:
        copy.wait()


def cast_down(steps, down_master, held):
    _, rows, hidden = down_master.shape
    count = len(steps)
    piece = jax.ShapeDtypeStruct((held, rows, hidden), jnp.bfloat16)
    return pl.pallas_call(
        functools.partial(cast_down_kernel, steps),
        in_specs=[ANYWHERE],
        out_specs=[ANYWHERE] * count,
        out_shape=[piece] * count,
        scratch_shapes=[
            pltpu.VMEM((count, *piece.shape), jnp.float32),
            pltpu.VMEM((count, *piece.shape), jnp.bfloat16),
            pltpu.SemaphoreType.DMA((count,)),
            pltpu.SemaphoreType.DMA((count,)),
        ],
        compiler_params=ROOM,
    )(down_master)


def column_of(expert, swap, hidden):
    return pl.multiple_of((expert * 4 + (lax.axis_index("tp") ^ swap)) * hidden, LANES)


def lay_pair_kernel(step, *refs):
    parts, (gate_out, up_out, held_buf, in_sem, out_sem) = refs[:4], refs[-5:]
    _, held, rows, hidden = parts[0].shape
    first = pl.multiple_of(sender(step) * rows, LANES)
    loads, stores = [], []
    for which in range(2):
        for swap, part in enumerate(parts):
            loads.append(
                pltpu.make_async_copy(
                    part.at[which], held_buf.at[which, swap], in_sem.at[which, swap]
                )
            )
            loads[-1].start()
    for which, out in enumerate((gate_out, up_out)):
        for swap in range(4):
            loads[which * 4 + swap].wait()
            for e in range(held):
                place = out.at[pl.ds(first, rows), pl.ds(column_of(e, swap, hidden), hidden)]
                stores.append(
                    pltpu.make_async_copy(
                        held_buf.at[which, swap, e], place, out_sem.at[which, swap, e]
                    )
                )
                stores[-1].start()
    for copy in stores:
        copy.wait()


def lay_pair(step, parts, outs, total):
    _, held, rows, hidden = parts[0].shape
    fresh = outs is None
    shape = jax.ShapeDtypeStruct((total, held * 4 * hidden), jnp.bfloat16)
    return pl.pallas_call(
        functools.partial(lay_pair_kernel, step),
        in_specs=[ANYWHERE] * (4 if fresh else 6),
        out_specs=[ANYWHERE, ANYWHERE],
        out_shape=[shape, shape],
        scratch_shapes=[
            pltpu.VMEM((2, 4, held, rows, hidden), jnp.bfloat16),
            pltpu.SemaphoreType.DMA((2, 4)),
            pltpu.SemaphoreType.DMA((2, 4, held)),
        ],
        input_output_aliases={} if fresh else {4: 0, 5: 1},
        compiler_params=ROOM,
    )(*parts, *(() if fresh else outs))


def lay_down_kernel(step, sums, factor, *refs):
    parts, scaled_ref, others = refs[:4], refs[4], refs[5 : 5 + sums]
    out, result_ref, held_buf, block, scaled_buf, sum_buf, in_sem, sum_sem, sems = refs[-9:]
    held, rows, hidden = parts[0].shape
    first = pl.multiple_of(sender(step) * rows, LANES)
    half, width = held // 2, scaled_buf.shape[1] // 2
    loads = []
    for side in range(2):
        experts, columns = pl.ds(side * half, half), pl.ds(side * width, width)
        for swap, part in enumerate(parts):
            place = held_buf.at[swap, experts]
            loads.append(
                pltpu.make_async_copy(part.at[experts], place, in_sem.at[side, swap])
            )
        place = scaled_buf.at[:, columns]
        loads.append(pltpu.make_async_copy(scaled_ref.at[:, columns], place, sems.at[side]))
    for i, other in enumerate(others):
        loads.append(pltpu.make_async_copy(other, sum_buf.at[i], sum_sem.at[i]))
    for copy in loads:
        copy.start()
    product, stores = None, []
    for side in range(2):
        columns = pl.ds(side * width, width)
        for swap in range(4):
            loads[side * 5 + swap].wait()
            for e in range(side * half, (side + 1) * half):
                block[:, pl.ds(column_of(e, swap, hidden), hidden)] = held_buf[swap, e]
        place = out.at[pl.ds(first, rows), columns]
        stores.append(pltpu.make_async_copy(block.at[:, columns], place, sems.at[2 + side]))
        stores[side].start()
        loads[side * 5 + 4].wait()
        dot = lax.dot_general(
            scaled_buf[:, columns],
            block[:, columns],
            (((1,), (1,)), ((), ())),
            preferred_element_type=jnp.float32,
        )
        product = dot if product is None else product + dot
    if sums:
        for i in range(sums):
            loads[10 + i].wait()
            product += sum_buf[i].astype(jnp.float32)
        product *= factor
    result_ref[...] = product.astype(result_ref.dtype)
    for copy in stores:
        copy.wait()


def lay_down(step, parts, scaled, others, out, total):
    held, rows, hidden = parts[0].shape
    width = held * 4 * hidden
    tokens = scaled.shape[0]
    fresh = out is None
    sums = len(others)
    return pl.pallas_call(
        functools.partial(lay_down_kernel, step, sums, FF ** (-0.5)),
        in_specs=[ANYWHERE] * (5 + sums + (0 if fresh else 1)),
        out_specs=[ANYWHERE, pl.BlockSpec(memory_space=pltpu.VMEM)],
        out_shape=[
            jax.ShapeDtypeStruct((total, width), jnp.bfloat16),
            jax.ShapeDtypeStruct((tokens, rows), jnp.bfloat16),
        ],
        scratch_shapes=[
            pltpu.VMEM((4, held, rows, hidden), jnp.bfloat16),
            pltpu.VMEM((rows, width), jnp.bfloat16),
            pltpu.VMEM((tokens, width), jnp.bfloat16),
            pltpu.VMEM((max(sums, 1), tokens, rows), jnp.bfloat16),
            pltpu.SemaphoreType.DMA((2, 4)),
            pltpu.SemaphoreType.DMA((max(sums, 1),)),
            pltpu.SemaphoreType.DMA((4,)),
        ],
        input_output_aliases={} if fresh else {5 + sums: 0},
        compiler_params=ROOM,
    )(*parts, scaled, *others, *(() if fresh else (out,)))


def ready_kernel(held, prompt_ref, group_ref, inner_ref, route_ref, normed_ref, weight_ref):
    values = prompt_ref[...].astype(jnp.float32)
    mean = jnp.mean(values * values, axis=1, keepdims=True)
    normed_ref[...] = (values * lax.rsqrt(mean + 1e-06)).astype(jnp.bfloat16)
    chosen = group_ref[...] * EPG + inner_ref[...]
    for e in range(held):
        owner = lax.axis_index("fs") * held + e
        picked = jnp.where(chosen == owner, route_ref[...], 0.0)
        row = jnp.sum(picked, axis=0, keepdims=True)
        weight_ref[e] = jnp.broadcast_to(row, (LANES, row.shape[1])).T


def ready(prompt, group_choice, inner_choice, route_weight, held):
    tokens = prompt.shape[0]
    near = pl.BlockSpec(memory_space=pltpu.VMEM)
    return pl.pallas_call(
        functools.partial(ready_kernel, held),
        in_specs=[near] * 4,
        out_specs=[near] * 2,
        out_shape=[
            jax.ShapeDtypeStruct(prompt.shape, jnp.bfloat16),
            jax.ShapeDtypeStruct((held, tokens, LANES), jnp.float32),
        ],
        compiler_params=ROOM,
    )(prompt, group_choice[None, :], inner_choice.T, route_weight.T)


def act_kernel(normed_ref, gate_ref, up_ref, weight_ref, out_ref):
    normed = normed_ref[...]
    factor = normed.shape[1] ** (-0.5)
    gate = jnp.dot(normed, gate_ref[...], preferred_element_type=jnp.float32) * factor
    up = jnp.dot(normed, up_ref[...], preferred_element_type=jnp.float32) * factor
    weight = jnp.concatenate([weight_ref[0]] * (gate.shape[1] // LANES), axis=1)
    out_ref[...] = (weight * (gate / (1.0 + jnp.exp(-gate))) * up).astype(jnp.bfloat16)


def act(normed, gate_local, up_local, weight):
    tokens, width = normed.shape
    held = weight.shape[0]
    block = gate_local.shape[1] // held
    columns = pl.BlockSpec((width, block), lambda e: (0, e))
    return pl.pallas_call(
        act_kernel,
        grid=(held,),
        in_specs=[
            pl.BlockSpec(normed.shape, lambda e: (0, 0)),
            columns,
            columns,
            pl.BlockSpec((1, tokens, LANES), lambda e: (e, 0, 0)),
        ],
        out_specs=pl.BlockSpec((tokens, block), lambda e: (0, e)),
        out_shape=jax.ShapeDtypeStruct((tokens, held * block), jnp.bfloat16),
        compiler_params=ROOM,
    )(normed, gate_local, up_local, weight)


def fs_send(value, offset, sign):
    ways = lax.axis_size("fs")
    chips = offset[0] if sign > 0 else ways // 2 - offset[0]
    pairs = [
        (i, (i // 2 + chips) % (ways // 2) * 2 + (i % 2 ^ offset[1])) for i in range(ways)
    ]
    return lax.ppermute(value, "fs", pairs)


def tp_swap(value, step):
    return lax.ppermute(value, "tp", [(i, i ^ step) for i in range(lax.axis_size("tp"))])


def plan(ways):
    chips = ways // 2
    apart = []
    for near in range(1, chips // 2 + 1):
        both = [near] if 2 * near == chips else [near, chips - near]
        apart += [(far, core) for core in range(2) for far in both]
    pair = [(False, offset) for offset in [(0, 0), (0, 1)] + apart]
    apart.sort(key=lambda offset: -min(offset[0], chips - offset[0]))
    return pair + [(True, offset) for offset in apart + [(0, 1), (0, 0)]]


def turns(pieces):
    seen = {True: 0, False: 0}
    result = []
    for down, _ in pieces:
        result.append(seen[down] % 2 == 0)
        seen[down] += 1
    return result


def exchange_shards(
    prompt, norm_gain, gate_master, up_master, down_master, group_choice, inner_choice, route_weight
):
    ways = lax.axis_size("fs")
    experts, rows, _ = gate_master.shape
    held, total = experts // ways, rows * ways
    pieces = plan(ways)

    cast = cast_pairs((HERE,), norm_gain, gate_master, up_master, held)
    others = tuple(offset for down, offset in pieces[1:] if not down)
    cast += cast_pairs(others, norm_gain, gate_master, up_master, held)
    normed, weight = ready(prompt, group_choice, inner_choice, route_weight, held)
    cast += cast_down(tuple(offset for down, offset in pieces if down), down_master, held)

    own, left, right, last = ({}, {}, {}, {})
    turn = turns(pieces)
    for index, (down, step) in enumerate(pieces):
        piece = cast[index]
        if step != HERE:
            piece = fs_send(piece, step, 1)
        own[index] = piece
        left[index] = tp_swap(piece, 1)
        right[index] = tp_swap(piece, 2)
        last[index] = tp_swap(left[index], 2) if turn[index] else tp_swap(right[index], 1)

    pair_out, down_out, scaled, sums = None, None, None, ()
    for index, (down, step) in enumerate(pieces):
        parts = own[index], left[index], right[index], last[index]
        if not down:
            pair_out = lay_pair(step, parts, pair_out, total)
            continue
        if scaled is None:
            scaled = act(normed, *pair_out, weight)
        down_out, result = lay_down(
            step, parts, scaled, sums if step == HERE else (), down_out, total
        )
        if step != HERE:
            sums += (fs_send(result, step, -1),)
    return (*pair_out, down_out, result)


def solution(mesh):
    in_specs = (
        P("tp", None),
        P("fs"),
        P(None, "fs", "tp"),
        P(None, "fs", "tp"),
        P(None, "fs", "tp"),
        P("tp"),
        P("tp", None),
        P("tp", None),
    )
    out_specs = (P(None, "fs"), P(None, "fs"), P(None, "fs"), P("tp", "fs"))
    wrap = functools.partial(
        jax.shard_map, mesh=mesh, in_specs=in_specs, out_specs=out_specs, check_vma=False
    )
    ways, parts = mesh.shape["fs"], mesh.shape["tp"]
    whole_experts = ways & (ways - 1) == 0 and ways >= 4 and (GROUPS * EPG) % (2 * ways) == 0
    if not (whole_experts and parts == 4 and FF % (parts * LANES) == 0):
        return wrap(general_shards)

    return wrap(exchange_shards)
```
